32 devices in a mesh: ep: 8 (over z, x), tp: 4 (over y, core).
Axes of the slice: x: 2, y: 2, z: 4, core: 2. Of those that a mesh axis runs over, the one named last changes fastest.
Arguments:
- mixer_tokens: bfloat16 [1536, 2048], P('ep'), may hold values from -6 to 6
- mixer_gain: float32 [2048], replicated, may hold values from 0.1 to 1.9
- query_weight: bfloat16 [1024, 2048], P('tp'), may hold values from -1 to 1
- key_weight: bfloat16 [1024, 2048], P('tp'), may hold values from -1 to 1
- value_weight: bfloat16 [1024, 2048], P('tp'), may hold values from -0.125 to 0.125
- forget_weight: bfloat16 [2048, 16], P(None, 'tp'), may hold values from -0.125 to 0.125
- forget_bias: float32 [8, 16], P('ep', 'tp'), may hold values from 2.98 to 10.4
- output_weight: bfloat16 [1024, 2048], P(None, 'tp'), may hold values from -0.1875 to 0.1875
- expert_tokens: bfloat16 [1024, 2048], P('ep'), may hold values from -6 to 6
- expert_gain: float32 [2048], replicated, may hold values from 0.1 to 1.9
- routes: int32 [1024, 2], P('ep'), may hold values from 0 to 7, all different within a row; in each aligned block of 128 rows (0 to 127, 128 to 255, ...) at most 64 rows name the same one
- route_weights: float32 [1024, 2], P('ep'), may hold values from 0.2 to 1
- gate_weight: bfloat16 [8, 3584, 2048], P('ep', 'tp'), may hold values from -0.125 to 0.125
- up_weight: bfloat16 [8, 3584, 2048], P('ep', 'tp'), may hold values from -0.125 to 0.125
- down_weight: bfloat16 [8, 3584, 2048], P('ep', 'tp'), may hold values from -0.09375 to 0.09375
Outputs:
- mixer_output: bfloat16 [1536, 2048], P('ep', 'tp')
- expert_output: bfloat16 [1024, 2048], P('ep', 'tp')
The draws below stay inside these ranges and needn't reach their ends.
Inputs may be any that keep to these rules, and one draw needn't show every extreme that they name: `routes`: within the tokens of one index of ep (aligned blocks of 128 rows) no expert is named more than 64 times, a bound that some block reaches; the 2 experts of a token differ.
All inputs are finite; a program needn't handle non-finite values.
Results may differ from the reference program's by a relative error of at most 0.019.
Values may be sent and summed in bfloat16 or wider, within the bound.
A program may use at most 128 MiB of HBM per device.

```python
import math
import jax
import jax.numpy as jnp
import numpy as np
from jax import lax

D = 2048
HEADS = 16
HD = 64
EXPERT_FF = 3584
TOP = 2
TOK_A = 192
TOK_B = 128
EXPERTS = 8
CAP = 64
TOKENS_A = 1536
TOKENS_B = 1024
N_EP = 8
N_TP = 4


def spiked_weight(key, salt):
    base_draw = jax.random.normal(jax.random.fold_in(key, salt), (HEADS * HD, D), jnp.float32)
    base_draw = jnp.clip(base_draw, -6.0, 6.0) * D ** (-0.5)
    return base_draw.astype(jnp.bfloat16)


def draw_query_weight(key, part):
    return spiked_weight(key, 11)


def draw_key_weight(key, part):
    return spiked_weight(key, 12)


def draw_mixer_tokens(key, part):
    values = jnp.clip(jax.random.normal(jax.random.fold_in(key, 201), (TOKENS_A, D), jnp.float32), -6.0, 6.0)
    return values.astype(jnp.bfloat16)


def draw_forget_bias(key, part):
    block_count = TOKENS_A // TOK_A
    chance = 0.5
    slow_heads = jax.random.bernoulli(jax.random.fold_in(key, 301), chance, (HEADS,))
    base_level = jnp.where(slow_heads, 9.7, math.log(40.0)).astype(jnp.float32)
    block_drift = jax.random.uniform(jax.random.fold_in(key, 302), (block_count, HEADS), jnp.float32, -0.7, 0.7)
    return base_level[None, :] + block_drift


def steps_of(rng, shape, split, least, largest):
    factor_of = 1.0
    for axis_at, blocks in split:
        draws = jax.random.uniform(jax.random.fold_in(jax.random.fold_in(rng, 6), axis_at), (blocks,), jnp.float32, least / len(split), largest / len(split))
        factor_of = factor_of * jnp.repeat(jnp.exp(draws), shape[axis_at] // blocks).reshape((-1,) + (1,) * (len(shape) - 1 - axis_at))
    return factor_of


def deal_out(rng, own, number, rows, count, top, limit, lean):
    order = jax.random.permutation(rng, count)
    heavy_load, common = portions_of(count, rows * top, limit, lean, True), portions_of(count, rows * top, limit, lean, False)
    places = jnp.arange(count)

    def named(tallies, offset_by):
        used = int((tallies > 0).sum())
        fixed = max(1, used // 4)
        moved = fixed + (places - fixed + offset_by * (used - fixed)) % max(1, count - fixed)
        return jnp.zeros((count,), jnp.int32).at[order[jnp.where(places < fixed, places, moved)]].set(jnp.asarray(tallies, jnp.int32))

    tallies = jnp.where(number % 4 == 0, named(heavy_load, number // 4), named(common, number - number // 4 - 1))
    mixed = jax.random.permutation(jax.random.fold_in(own, 3), count)
    source_of, sink = mixed[0:count // 2 * 2:2], mixed[1:count // 2 * 2:2]
    margin = jnp.minimum(tallies[source_of] - 1, limit - tallies[sink]) // 2
    margin = jnp.where((source_of == order[0]) | (sink == order[0]) | (tallies[sink] == 0), 0, jnp.maximum(margin, 0))
    moved = jax.random.randint(jax.random.fold_in(own, 4), (count // 2,), 0, 1 << 20) % (margin + 1)
    tallies = tallies.at[source_of].add(-moved).at[sink].add(moved)
    members = jnp.searchsorted(jnp.cumsum(tallies), jnp.arange(rows * top), side="right").astype(jnp.int32)
    listing = members.reshape(top, rows).T
    listing = listing[jax.random.permutation(jax.random.fold_in(own, 1), rows)]
    offset_by = jax.random.randint(jax.random.fold_in(own, 2), (rows, 1), 0, top)
    return jnp.take_along_axis(listing, (jnp.arange(top)[None, :] + offset_by) % top, axis=1)


def portions_of(count, total, most, lean, full):
    loads = [(1 << 20) // math.isqrt(grade ** lean) + 1 for grade in range(1, count + 1)]
    largest = most if full else min(most, max(-(-total // count), total * loads[0] // sum(loads)))
    least = 1 if total - largest >= count - 1 else 0
    given, rest = [largest] + [least] * (count - 1), total - largest - least * (count - 1)
    while rest > 0:
        free = [i for i in range(1, count) if given[i] < largest] or [i for i in range(1, count) if given[i] < most]
        mass, remaining = sum([loads[i] for i in free]), rest
        for i in free:
            extra = min(most - given[i], max(1, remaining * loads[i] // mass), rest)
            given[i] = given[i] + extra
            rest = rest - extra
    return np.array(given)


def centred(rng, dims, width, most, cuts=(), kind=jnp.bfloat16):
    values = jax.random.normal(rng, dims, jnp.float32) * width
    if len(cuts) > 0:
        values = steps_of(rng, dims, cuts, -0.22, 0.18) * values
    return jnp.clip(values, min=-most, max=most).astype(kind)


def setup_inputs(seed: int = 0) -> dict:
    splits = jax.random.split(jax.random.key(seed), 16)
    mixer_tokens = draw_mixer_tokens(jax.random.fold_in(splits[15], 71), 0)
    mixer_gain = jnp.clip(1.0 + 0.18 * jax.random.normal(splits[1], (D,), jnp.float32), 0.1, 1.9)
    query_weight = draw_query_weight(jax.random.fold_in(splits[15], 71), 0)
    key_weight = draw_key_weight(jax.random.fold_in(splits[15], 71), 0)
    value_weight = centred(splits[4], (HEADS * HD, D), D ** -0.5, 0.125, ((0, 4),))
    forget_weight = centred(splits[5], (D, HEADS), D ** -0.5, 0.125, ((1, 4),))
    forget_bias = draw_forget_bias(jax.random.fold_in(splits[15], 71), 0)
    output_weight = centred(splits[7], (HEADS * HD, D), (HEADS * HD) ** -0.5, 0.1875, ((1, 4),))
    expert_tokens = centred(splits[8], (TOKENS_B, D), 1.0, 6.0, ((0, 8),))
    expert_gain = jnp.clip(1.0 + 0.18 * jax.random.normal(splits[9], (D,), jnp.float32), 0.1, 1.9)
    routes_keys = jax.random.split(jax.random.fold_in(splits[10], 1), TOKENS_B // TOK_B)
    routes_turns = jax.random.permutation(jax.random.fold_in(splits[10], 3), TOKENS_B // TOK_B)
    routes = jax.vmap(lambda own, number: deal_out(jax.random.fold_in(splits[10], 2), own, number, TOK_B, EXPERTS, TOP, CAP, 2))(routes_keys, routes_turns).reshape((TOKENS_B, TOP))
    route_weights = jnp.clip(0.2 + 0.8 * jax.random.uniform(splits[11], (TOKENS_B, TOP), jnp.float32) ** steps_of(splits[11], (TOKENS_B, TOP), ((0, 8),), -0.2, 0.2), 0.2, 1.0)
    gate_weight = centred(splits[12], (EXPERTS, EXPERT_FF, D), D ** -0.5, 0.125, ((0, 8), (1, 4)))
    up_weight = centred(splits[13], (EXPERTS, EXPERT_FF, D), D ** -0.5, 0.125, ((0, 8), (1, 4)))
    down_weight = centred(splits[14], (EXPERTS, EXPERT_FF, D), EXPERT_FF ** -0.5, 0.09375, ((0, 8), (1, 4)))
    return {"mixer_tokens": mixer_tokens, "mixer_gain": mixer_gain, "query_weight": query_weight, "key_weight": key_weight, "value_weight": value_weight, "forget_weight": forget_weight, "forget_bias": forget_bias, "output_weight": output_weight, "expert_tokens": expert_tokens, "expert_gain": expert_gain, "routes": routes, "route_weights": route_weights, "gate_weight": gate_weight, "up_weight": up_weight, "down_weight": down_weight}


MEAN_FLOOR = 0.1
HEAD_FLOOR = 1.0

def normed_rows(inputs, gain):
    values = inputs.astype(jnp.float32)
    square = lax.optimization_barrier(jnp.mean(values * values, axis=-1, keepdims=True))
    return (values * lax.rsqrt(jnp.maximum(square, MEAN_FLOOR)) * gain).astype(jnp.bfloat16)

def by_rows(left, weight):
    return lax.dot_general(left, weight, (((1,), (1,)), ((), ())), preferred_element_type=jnp.float32)

def reference(mixer_tokens, mixer_gain, query_weight, key_weight, value_weight, forget_weight, forget_bias, output_weight, expert_tokens, expert_gain, routes, route_weights, gate_weight, up_weight, down_weight):
    sequence = mixer_tokens.shape[0]
    normed = normed_rows(mixer_tokens, mixer_gain)
    queries = by_rows(normed, query_weight).astype(jnp.bfloat16)
    key_rows = by_rows(normed, key_weight).astype(jnp.bfloat16)
    value_rows = by_rows(normed, value_weight).astype(jnp.bfloat16)
    pre_gate = jnp.dot(normed, forget_weight, preferred_element_type=jnp.float32)
    pre_gate = pre_gate + jnp.repeat(forget_bias, TOK_A, axis=0)
    cumulative = jnp.cumsum(jax.nn.log_sigmoid(pre_gate), axis=0)
    head_query = queries.reshape(sequence, HEADS, HD).astype(jnp.float32)
    head_keys = key_rows.reshape(sequence, HEADS, HD).astype(jnp.float32)
    head_values = value_rows.reshape(sequence, HEADS, HD).astype(jnp.float32)
    key_pos = jnp.arange(sequence, dtype=jnp.int32)

    def attend_block(number):
        first_row = (number * TOK_A).astype(jnp.int32)
        block_query = lax.dynamic_slice_in_dim(head_query, first_row, TOK_A, 0)
        block_cum = lax.dynamic_slice_in_dim(cumulative, first_row, TOK_A, 0)
        scores = jnp.einsum('qhd,khd->hqk', block_query, head_keys) * HD ** (-0.5)
        scores = scores + block_cum.T[:, :, None] - cumulative.T[:, None, :]
        query_pos = first_row + jnp.arange(TOK_A, dtype=jnp.int32)
        scores = jnp.where(key_pos[None, None, :] <= query_pos[None, :, None], scores, -jnp.inf)
        row_max = lax.optimization_barrier(jnp.max(scores, axis=-1, keepdims=True))
        weights = lax.optimization_barrier(jnp.exp(scores - row_max).astype(jnp.bfloat16)).astype(jnp.float32)
        attended = jnp.einsum('hqk,khd->qhd', weights, head_values)
        attended = attended * lax.rsqrt(lax.optimization_barrier(jnp.mean(attended * attended, axis=-1, keepdims=True)) + HEAD_FLOOR)
        return attended.reshape(TOK_A, HEADS * HD).astype(jnp.bfloat16)
    head_out = lax.map(attend_block, jnp.arange(N_EP, dtype=jnp.int32)).reshape(sequence, HEADS * HD)
    mixer_output = jnp.dot(head_out, output_weight, preferred_element_type=jnp.float32).astype(jnp.bfloat16)
    expert_normed = normed_rows(expert_tokens, expert_gain).reshape(N_EP, TOK_B, D)
    flat_routes = routes.reshape(N_EP, TOK_B * TOP)
    onehot = (flat_routes[:, :, None] == jnp.arange(EXPERTS, dtype=jnp.int32)[None, None, :]).astype(jnp.int32)
    slot_rank = lax.optimization_barrier(jnp.sum((jnp.cumsum(onehot, axis=1) - 1) * onehot, axis=2)).astype(jnp.int32)
    slot_index = flat_routes * CAP + slot_rank
    token_of = jnp.arange(TOK_B * TOP, dtype=jnp.int32) // TOP
    source = jnp.broadcast_to(jnp.arange(N_EP, dtype=jnp.int32)[:, None], flat_routes.shape)
    outgoing = jnp.zeros((N_EP, EXPERTS * CAP, D), jnp.bfloat16)
    outgoing = outgoing.at[source, slot_index].set(expert_normed[source, token_of[None, :]])
    groups = EXPERT_FF // N_TP

    def run_expert(number):
        slot_rows = lax.dynamic_slice_in_dim(outgoing, (number * CAP).astype(jnp.int32), CAP, 1)
        slot_rows = slot_rows.reshape(N_EP * CAP, D)
        gate_act = by_rows(slot_rows, gate_weight[number])
        up_act = by_rows(slot_rows, up_weight[number])
        hidden = (jax.nn.silu(gate_act) * up_act).astype(jnp.bfloat16)
        partial_value = jnp.einsum('rtf,tfd->trd', hidden.reshape(N_EP * CAP, N_TP, groups).astype(jnp.float32), down_weight[number].reshape(N_TP, groups, D).astype(jnp.float32))
        partial_value = lax.optimization_barrier(partial_value.astype(jnp.bfloat16)).astype(jnp.float32)
        return lax.optimization_barrier(jnp.sum(partial_value, axis=0)).astype(jnp.bfloat16)
    results = lax.map(run_expert, jnp.arange(EXPERTS, dtype=jnp.int32))
    picked = results.reshape(EXPERTS, N_EP, CAP, D)[flat_routes, source, slot_rank]
    weighted = picked.astype(jnp.float32) * route_weights.reshape(N_EP, TOK_B * TOP)[:, :, None]
    expert_output = lax.optimization_barrier(jnp.sum(weighted.reshape(N_EP, TOK_B, TOP, D), axis=2))
    expert_output = expert_output.reshape(N_EP * TOK_B, D).astype(jnp.bfloat16)
    return (mixer_output, expert_output)
```

```python
import functools

import jax
import jax.numpy as jnp
from jax import lax
from jax.experimental import pallas as pl
from jax.experimental.pallas import tpu as pltpu
from jax.sharding import PartitionSpec as P

HD = 64
MEAN_FLOOR = 0.1
HEAD_FLOOR = 1.0
MESH = pl.DeviceIdType.MESH
VM = pl.BlockSpec(memory_space=pltpu.VMEM)
DMA = pltpu.SemaphoreType.DMA


def normed_rows(inputs, gain):
    values = inputs.astype(jnp.float32)
    square = jnp.mean(values * values, axis=-1, keepdims=True)
    return (values * lax.rsqrt(jnp.maximum(square, MEAN_FLOOR)) * gain).astype(jnp.bfloat16)


def by_rows(left, weight):
    return lax.dot_general(
        left, weight, (((1,), (1,)), ((), ())), preferred_element_type=jnp.float32
    )


class Place:
    def __init__(self, n_ep, n_tp):
        self.n_ep, self.n_tp, self.ny = n_ep, n_tp, n_tp // 2
        self.e = lax.axis_index("ep")
        self.t = lax.axis_index("tp")
        self.y, self.c = self.t // 2, self.t % 2
        self.partner = self.y * 2 + (1 - self.c)

    def ep(self, k):
        return (self.e + k) % self.n_ep

    def y_at(self, off):
        return (self.y + self.ny + off) % self.ny

    def chip(self, off):
        return self.y_at(off) * 2 + self.c

    def barrier(self):
        sem = pltpu.get_barrier_semaphore()
        for k in range(1, self.n_ep):
            pl.semaphore_signal(
                sem, inc=1, device_id={"ep": self.ep(k), "tp": self.t}, device_id_type=MESH
            )
        for off in range(1, self.ny):
            pl.semaphore_signal(
                sem, inc=1, device_id={"ep": self.e, "tp": self.chip(off)}, device_id_type=MESH
            )
        pl.semaphore_signal(
            sem, inc=1, device_id={"ep": self.e, "tp": self.partner}, device_id_type=MESH
        )
        pl.semaphore_wait(sem, self.n_ep - 1 + self.ny - 1 + 1)


def remote(src, dst, send, recv, e, t):
    return pltpu.make_async_remote_copy(
        src_ref=src,
        dst_ref=dst,
        send_sem=send,
        recv_sem=recv,
        device_id={"ep": e, "tp": t},
        device_id_type=MESH,
    )


class Exchange:
    def __init__(self, place, send, land, sems):
        self.p, self.send, self.land = place, send, land
        self.ssem, self.rsem = sems

    def copy(self, k):
        p = self.p
        d = p.ep(k)
        return remote(
            self.send(d), self.land(p.e), self.ssem.at[d], self.rsem.at[p.e], d, p.t
        )

    def arrival(self, k):
        p = self.p
        s = p.ep(k)
        return remote(self.send(s), self.land(s), self.ssem.at[s], self.rsem.at[s], s, p.t)

    def own(self):
        p = self.p
        return pltpu.make_async_copy(self.send(p.e), self.land(p.e), self.rsem.at[p.e])

    def start(self):
        for k in range(1, self.p.n_ep):
            self.copy(k).start()
        self.own().start()

    def wait_arrival(self, k):
        if k == 0:
            self.own().wait()
        else:
            self.arrival(k).wait_recv()

    def wait_sent(self):
        for k in range(1, self.p.n_ep):
            self.copy(k).wait_send()


class Spread:
    def __init__(self, place, land, sems):
        self.p, self.land = place, land
        self.ys, self.yr, self.ps, self.pr = sems

    def y_copy(self, off, s):
        p = self.p
        block = self.land(p.t, s)
        return remote(
            block, block, self.ys.at[off - 1, s], self.yr.at[off - 1, s], p.e, p.chip(off)
        )

    def y_arrival(self, off, s):
        p = self.p
        block = self.land(p.chip(-off), s)
        return remote(
            block, block, self.ys.at[off - 1, s], self.yr.at[off - 1, s], p.e, p.chip(-off)
        )

    def p_copy(self, off, s):
        p = self.p
        block = self.land(p.chip(-off), s)
        return remote(block, block, self.ps.at[off, s], self.pr.at[off, s], p.e, p.partner)

    def p_arrival(self, off, s):
        p = self.p
        block = self.land(p.y_at(-off) * 2 + (1 - p.c), s)
        return remote(block, block, self.ps.at[off, s], self.pr.at[off, s], p.e, p.partner)

    def first(self, s):
        for off in range(1, self.p.ny):
            self.y_copy(off, s).start()
        self.p_copy(0, s).start()

    def relay(self, s):
        for off in range(1, self.p.ny):
            self.y_arrival(off, s).wait_recv()
            self.p_copy(off, s).start()

    def finish(self, s):
        for off in range(self.p.ny):
            self.p_arrival(off, s).wait_recv()
            self.p_copy(off, s).wait_send()
        for off in range(1, self.p.ny):
            self.y_copy(off, s).wait_send()


def spread_sems(n_ep, n_tp):
    ny = n_tp // 2
    far = max(ny - 1, 1)
    return [DMA((far, n_ep)), DMA((far, n_ep)), DMA((ny, n_ep)), DMA((ny, n_ep))]


def outward_kernel(
    n_ep, n_tp, slots, message, gates, out, message_out, gates_out,
    s0, s1, m0, m1, g0, g1, ys, yr, ps, pr,
):
    p = Place(n_ep, n_tp)
    width = slots.shape[2]

    def land(t, s):
        return out.at[s, :, pl.ds(pl.multiple_of(t * width, width), width)]

    p.barrier()
    slot_move = Exchange(p, lambda d: slots.at[d], lambda s: land(p.t, s), (s0, s1))
    gate_move = Exchange(p, lambda d: gates.at[d], lambda s: gates_out.at[s], (g0, g1))
    message_move = Exchange(p, lambda d: message.at[d], lambda s: message_out.at[s], (m0, m1))
    spread = Spread(p, land, (ys, yr, ps, pr))
    slot_move.start()
    gate_move.start()
    message_move.start()
    for k in range(n_ep):
        slot_move.wait_arrival(k)
        spread.first(p.ep(k))
    for k in range(n_ep):
        spread.relay(p.ep(k))
    for k in range(n_ep):
        gate_move.wait_arrival(k)
        message_move.wait_arrival(k)
        spread.finish(p.ep(k))
    slot_move.wait_sent()
    gate_move.wait_sent()
    message_move.wait_sent()


def homeward_kernel(
    n_ep, n_tp, partial, heads, ret, heads_all,
    pair, mine, out_y, in_y, final,
    h0, h1, a0, a1, r0, r1, q0, q1, ys, yr, ps, pr,
):
    p = Place(n_ep, n_tp)
    ny = p.ny
    width = ret.shape[2]

    def cols(t):
        return pl.ds(pl.multiple_of(t * width, width), width)

    def land(t, s):
        return heads_all.at[t, s]

    p.barrier()
    head_move = Exchange(p, lambda d: heads.at[d], lambda s: land(p.t, s), (h0, h1))
    spread = Spread(p, land, (ys, yr, ps, pr))
    head_move.start()

    def pair_copy(s, off):
        src = partial.at[s, :, cols(p.y_at(off) * 2 + (1 - p.c))]
        return remote(src, pair.at[s, off], r0.at[s, off], r1.at[s, off], p.e, p.partner)

    def y_copy(s, off, to):
        return remote(
            out_y.at[s, off - 1], in_y.at[s, off - 1],
            q0.at[s, off - 1], q1.at[s, off - 1], p.e, p.chip(to),
        )

    def final_copy(k):
        d = p.ep(k)
        return remote(final.at[d], ret.at[p.e], a0.at[d], a1.at[p.e], d, p.t)

    order = list(range(1, n_ep)) + [0]
    for k in order:
        for off in range(ny):
            pair_copy(p.ep(k), off).start()
    for k in order:
        s = p.ep(k)
        for off in [*range(1, ny), 0]:
            pair_copy(s, off).wait_recv()
            both = partial[s, :, cols(p.chip(off))].astype(jnp.float32) + pair[s, off].astype(
                jnp.float32
            )
            if off == 0:
                mine[s] = both
            else:
                out_y[s, off - 1] = both.astype(jnp.bfloat16)
                y_copy(s, off, off).start()
    for k in range(n_ep):
        head_move.wait_arrival(k)
        spread.first(p.ep(k))
    for k in order:
        s = p.ep(k)
        total = mine[s]
        for off in range(1, ny):
            y_copy(s, off, -off).wait_recv()
            total = total + in_y[s, off - 1].astype(jnp.float32)
        if k == 0:
            ret[s] = total.astype(jnp.bfloat16)
        else:
            final[s] = total.astype(jnp.bfloat16)
            final_copy(k).start()
    for k in range(n_ep):
        spread.relay(p.ep(k))
    for k in range(n_ep):
        spread.finish(p.ep(k))
    for k in range(n_ep):
        s = p.ep(k)
        for off in range(ny):
            pair_copy(s, off).wait_send()
        for off in range(1, ny):
            y_copy(s, off, off).wait_send()
    for k in range(1, n_ep):
        s = p.ep(k)
        remote(final.at[s], ret.at[s], a0.at[s], a1.at[s], s, p.t).wait_recv()
        final_copy(k).wait_send()
    head_move.wait_sent()


def outward(slots, message, gates, n_ep, n_tp):
    _, capacity, width = slots.shape
    sems = [DMA((n_ep,))] * 6 + spread_sems(n_ep, n_tp)
    return pl.pallas_call(
        functools.partial(outward_kernel, n_ep, n_tp),
        out_shape=[
            jax.ShapeDtypeStruct((n_ep, capacity, width * n_tp), slots.dtype),
            jax.ShapeDtypeStruct(message.shape, message.dtype),
            jax.ShapeDtypeStruct(gates.shape, gates.dtype),
        ],
        in_specs=[VM] * 3,
        out_specs=[VM] * 3,
        scratch_shapes=sems,
        compiler_params=pltpu.CompilerParams(collective_id=0, has_side_effects=True),
        name="outward",
    )(slots, message, gates)


def homeward(partial, heads, n_ep, n_tp):
    _, capacity, features = partial.shape
    width, ny = features // n_tp, n_tp // 2
    far = max(ny - 1, 1)
    scratch = [
        pltpu.VMEM((n_ep, ny, capacity, width), jnp.bfloat16),
        pltpu.VMEM((n_ep, capacity, width), jnp.float32),
        pltpu.VMEM((n_ep, far, capacity, width), jnp.bfloat16),
        pltpu.VMEM((n_ep, far, capacity, width), jnp.bfloat16),
        pltpu.VMEM((n_ep, capacity, width), jnp.bfloat16),
    ]
    sems = [DMA((n_ep,))] * 4 + [DMA((n_ep, ny))] * 2 + [DMA((n_ep, far))] * 2
    return pl.pallas_call(
        functools.partial(homeward_kernel, n_ep, n_tp),
        out_shape=[
            jax.ShapeDtypeStruct((n_ep, capacity, width), jnp.bfloat16),
            jax.ShapeDtypeStruct((n_tp,) + heads.shape, jnp.bfloat16),
        ],
        in_specs=[VM] * 2,
        out_specs=[VM] * 2,
        scratch_shapes=scratch + sems + spread_sems(n_ep, n_tp),
        compiler_params=pltpu.CompilerParams(collective_id=1, has_side_effects=True),
        name="homeward",
    )(partial, heads)


def on_device(
    mixer_tokens,
    mixer_gain,
    query_weight,
    key_weight,
    value_weight,
    forget_weight,
    forget_bias,
    output_weight,
    expert_tokens,
    expert_gain,
    routes,
    route_weights,
    gate_weight,
    up_weight,
    down_weight,
):
    n_ep, n_tp = lax.axis_size("ep"), lax.axis_size("tp")
    rows, features = mixer_tokens.shape
    local_heads = forget_weight.shape[1]
    share = n_ep // local_heads
    part = rows // share
    width = features // n_tp
    bf16, f32 = jnp.bfloat16, jnp.float32

    expert_normed = normed_rows(expert_tokens, expert_gain)
    token_count, top_count = routes.shape
    capacity = 2 * top_count * token_count // n_ep
    pairs = token_count * top_count
    flat_routes = routes.reshape(-1)
    onehot = flat_routes[:, None] == jnp.arange(n_ep, dtype=jnp.int32)[None, :]
    before = jnp.tril(jnp.ones((pairs, pairs), bf16), -1)
    ranks = jnp.dot(before, onehot.astype(bf16), preferred_element_type=f32)
    slot_rank = jnp.sum(jnp.where(onehot, ranks, 0.0), axis=1).astype(jnp.int32)
    slot_index = (flat_routes * capacity + slot_rank).reshape(token_count, top_count)
    slot_ids = jnp.arange(n_ep * capacity, dtype=jnp.int32)
    picks = [(slot_index[:, j][:, None] == slot_ids[None, :]).astype(bf16) for j in range(top_count)]
    column = lax.axis_index("tp") * width
    own_columns = lax.dynamic_slice_in_dim(expert_normed, column, width, 1)
    slots = lax.dot_general(
        sum(picks[1:], picks[0]), own_columns, (((0,), (0,)), ((), ())),
        preferred_element_type=f32,
    ).astype(bf16).reshape(n_ep, capacity, width)

    normed = normed_rows(mixer_tokens, mixer_gain)
    queries = by_rows(normed, query_weight).astype(bf16)
    key_rows = by_rows(normed, key_weight).astype(bf16)
    value_rows = by_rows(normed, value_weight).astype(bf16)
    pre_gate = jnp.dot(normed, forget_weight, preferred_element_type=f32) + forget_bias
    block_cum = jnp.dot(
        jnp.tril(jnp.ones((rows, rows), f32)), jax.nn.log_sigmoid(pre_gate),
        precision=lax.Precision.HIGHEST, preferred_element_type=f32,
    )
    key_value = jnp.concatenate(
        [
            key_rows.reshape(rows, local_heads, HD).transpose(1, 0, 2),
            value_rows.reshape(rows, local_heads, HD).transpose(1, 0, 2),
        ],
        axis=2,
    )
    key_value = jnp.broadcast_to(
        key_value[:, None], (local_heads, share, rows, 2 * HD)
    ).reshape(n_ep, rows, 2 * HD)
    half = part // 2
    query_parts = queries.reshape(share, 2, half, local_heads, HD).transpose(3, 0, 2, 1, 4)
    query_parts = query_parts.reshape(n_ep, half, 2 * HD)
    message = jnp.concatenate([key_value, query_parts], axis=1)
    gates = jnp.broadcast_to(block_cum.T[:, None, None, :], (local_heads, share, 1, rows))
    gates = gates.reshape(n_ep, 1, rows)

    all_slots, all_messages, all_gates = outward(slots, message, gates, n_ep, n_tp)

    positions = n_ep * rows
    all_gates = all_gates.reshape(n_ep, rows)
    totals = all_gates[:, rows - 1]
    lower = jnp.arange(n_ep)[None, :] < jnp.arange(n_ep)[:, None]
    base = jnp.sum(jnp.where(lower, totals[None, :], 0.0), axis=1)
    cumulative = all_gates + base[:, None]
    keys = all_messages[:, :rows, :HD].reshape(positions, HD)
    values = all_messages[:, :rows, HD:].reshape(positions, HD)
    head_query = all_messages[:, rows:].reshape(n_ep, half, 2, HD).transpose(0, 2, 1, 3)
    head_query = head_query.reshape(n_ep * part, HD)
    first = (lax.axis_index("ep") % share) * part
    query_cum = lax.dynamic_slice_in_dim(cumulative, first, part, 1).reshape(-1)
    query_pos = (
        jnp.arange(n_ep, dtype=jnp.int32)[:, None] * rows
        + first
        + jnp.arange(part, dtype=jnp.int32)[None, :]
    ).reshape(-1)
    key_pos = jnp.arange(positions, dtype=jnp.int32)
    scores = by_rows(head_query, keys) * HD ** (-0.5)
    scores = scores + query_cum[:, None] - cumulative.reshape(-1)[None, :]
    scores = jnp.where(key_pos[None, :] <= query_pos[:, None], scores, -jnp.inf)
    weights = jnp.exp(scores - jnp.max(scores, axis=-1, keepdims=True)).astype(bf16)
    attended = jnp.dot(weights, values, preferred_element_type=f32)
    rescale = lax.rsqrt(jnp.mean(attended * attended, axis=-1, keepdims=True) + HEAD_FLOOR)
    head_out = (attended * rescale).astype(bf16).reshape(n_ep, part, HD)

    flat_rows = all_slots.reshape(n_ep * capacity, features)
    gate_act = by_rows(flat_rows, gate_weight[0])
    up_act = by_rows(flat_rows, up_weight[0])
    hidden = (jax.nn.silu(gate_act) * up_act).astype(bf16)
    partial = jnp.dot(hidden, down_weight[0], preferred_element_type=f32).astype(bf16)
    partial = partial.reshape(n_ep, capacity, features)

    returned, heads_all = homeward(partial, head_out, n_ep, n_tp)

    heads_all = heads_all.reshape(n_tp, local_heads, share, part, HD).transpose(2, 3, 0, 1, 4)
    heads_all = heads_all.reshape(rows, n_tp * local_heads * HD)
    mixer_output = jnp.dot(heads_all, output_weight, preferred_element_type=f32).astype(bf16)
    returned = returned.reshape(n_ep * capacity, width)
    expert_output = 0.0
    for j in range(top_count):
        picked = jnp.dot(picks[j], returned, preferred_element_type=f32)
        expert_output = expert_output + picked * route_weights[:, j][:, None]
    return (mixer_output, expert_output.astype(bf16))


def solution(mesh):
    in_specs = (
        P("ep", None),
        P(),
        P("tp", None),
        P("tp", None),
        P("tp", None),
        P(None, "tp"),
        P("ep", "tp"),
        P(None, "tp"),
        P("ep", None),
        P(),
        P("ep", None),
        P("ep", None),
        P("ep", "tp", None),
        P("ep", "tp", None),
        P("ep", "tp", None),
    )
    out_specs = (P("ep", "tp"), P("ep", "tp"))
    return jax.shard_map(
        on_device, mesh=mesh, in_specs=in_specs, out_specs=out_specs, check_vma=False
    )
```

```python
import functools

import jax
import jax.numpy as jnp
from jax import lax
from jax.experimental import pallas as pl
from jax.experimental.pallas import tpu as pltpu
from jax.sharding import PartitionSpec as P

HD = 64
MEAN_FLOOR = 0.1
HEAD_FLOOR = 1.0
MESH = pl.DeviceIdType.MESH
VM = pl.BlockSpec(memory_space=pltpu.VMEM)
ANY = pl.BlockSpec(memory_space=pl.ANY)
DMA = pltpu.SemaphoreType.DMA


def normed_rows(inputs, gain):
    values = inputs.astype(jnp.float32)
    square = jnp.mean(values * values, axis=-1, keepdims=True)
    return (values * lax.rsqrt(jnp.maximum(square, MEAN_FLOOR)) * gain).astype(jnp.bfloat16)


def by_rows(left, weight):
    return lax.dot_general(
        left, weight, (((1,), (1,)), ((), ())), preferred_element_type=jnp.float32
    )


class Place:
    def __init__(self, n_ep, n_tp):
        self.n_ep, self.n_tp, self.ny = n_ep, n_tp, n_tp // 2
        self.e = lax.axis_index("ep")
        self.t = lax.axis_index("tp")
        self.y, self.c = self.t // 2, self.t % 2
        self.partner = self.y * 2 + (1 - self.c)

    def ep(self, k):
        return (self.e + k) % self.n_ep

    def y_at(self, off):
        return (self.y + self.ny + off) % self.ny

    def chip(self, off):
        return self.y_at(off) * 2 + self.c

    def barrier(self):
        sem = pltpu.get_barrier_semaphore()
        for k in range(1, self.n_ep):
            pl.semaphore_signal(
                sem, inc=1, device_id={"ep": self.ep(k), "tp": self.t}, device_id_type=MESH
            )
        for off in range(1, self.ny):
            pl.semaphore_signal(
                sem, inc=1, device_id={"ep": self.e, "tp": self.chip(off)}, device_id_type=MESH
            )
        pl.semaphore_signal(
            sem, inc=1, device_id={"ep": self.e, "tp": self.partner}, device_id_type=MESH
        )
        pl.semaphore_wait(sem, self.n_ep - 1 + self.ny - 1 + 1)


def remote(src, dst, send, recv, e, t):
    return pltpu.make_async_remote_copy(
        src_ref=src,
        dst_ref=dst,
        send_sem=send,
        recv_sem=recv,
        device_id={"ep": e, "tp": t},
        device_id_type=MESH,
    )


class Exchange:
    def __init__(self, place, send, land, sems):
        self.p, self.send, self.land = place, send, land
        self.ssem, self.rsem = sems

    def copy(self, k):
        p = self.p
        d = p.ep(k)
        return remote(
            self.send(d), self.land(p.e), self.ssem.at[d], self.rsem.at[p.e], d, p.t
        )

    def arrival(self, k):
        p = self.p
        s = p.ep(k)
        return remote(self.send(s), self.land(s), self.ssem.at[s], self.rsem.at[s], s, p.t)

    def own(self):
        p = self.p
        return pltpu.make_async_copy(self.send(p.e), self.land(p.e), self.rsem.at[p.e])

    def start(self):
        for k in range(1, self.p.n_ep):
            self.copy(k).start()
        self.own().start()

    def wait_arrival(self, k):
        if k == 0:
            self.own().wait()
        else:
            self.arrival(k).wait_recv()

    def wait_sent(self):
        for k in range(1, self.p.n_ep):
            self.copy(k).wait_send()


class Spread:
    def __init__(self, place, land, sems):
        self.p, self.land = place, land
        self.ys, self.yr, self.ps, self.pr = sems

    def y_copy(self, off, s):
        p = self.p
        block = self.land(p.t, s)
        return remote(
            block, block, self.ys.at[off - 1, s], self.yr.at[off - 1, s], p.e, p.chip(off)
        )

    def y_arrival(self, off, s):
        p = self.p
        block = self.land(p.chip(-off), s)
        return remote(
            block, block, self.ys.at[off - 1, s], self.yr.at[off - 1, s], p.e, p.chip(-off)
        )

    def p_copy(self, off, s):
        p = self.p
        block = self.land(p.chip(-off), s)
        return remote(block, block, self.ps.at[off, s], self.pr.at[off, s], p.e, p.partner)

    def p_arrival(self, off, s):
        p = self.p
        block = self.land(p.y_at(-off) * 2 + (1 - p.c), s)
        return remote(block, block, self.ps.at[off, s], self.pr.at[off, s], p.e, p.partner)

    def first(self, s):
        for off in range(1, self.p.ny):
            self.y_copy(off, s).start()
        self.p_copy(0, s).start()

    def relay(self, s):
        for off in range(1, self.p.ny):
            self.y_arrival(off, s).wait_recv()
            self.p_copy(off, s).start()

    def finish(self, s):
        for off in range(self.p.ny):
            self.p_arrival(off, s).wait_recv()
        self.wait_sent(s)

    def wait_sent(self, s):
        for off in range(self.p.ny):
            self.p_copy(off, s).wait_send()
        for off in range(1, self.p.ny):
            self.y_copy(off, s).wait_send()


def spread_sems(n_ep, n_tp):
    ny = n_tp // 2
    far = max(ny - 1, 1)
    return [DMA((far, n_ep)), DMA((far, n_ep)), DMA((ny, n_ep)), DMA((ny, n_ep))]


def outward_kernel(
    n_ep, n_tp, slots, message, gates, gate_weight, up_weight,
    hidden, message_out, gates_out,
    out, gate_held, up_held, gate_act, up_act,
    s0, s1, m0, m1, g0, g1, w, ys, yr, ps, pr,
):
    p = Place(n_ep, n_tp)
    width = slots.shape[2]

    def cols(t):
        return pl.ds(pl.multiple_of(t * width, width), width)

    def land(t, s):
        return out.at[s, :, cols(t)]

    def multiply(t, opening):
        rows = out[:, :, cols(t)].reshape(hidden.shape[0], width)
        for held, total in ((gate_held, gate_act), (up_held, up_act)):
            product = by_rows(rows, held[:, cols(t)])
            total[...] = product if opening else total[...] + product

    loads = [
        pltpu.make_async_copy(gate_weight, gate_held, w.at[0]),
        pltpu.make_async_copy(up_weight, up_held, w.at[1]),
    ]
    for load in loads:
        load.start()
    p.barrier()
    slot_move = Exchange(p, lambda d: slots.at[d], lambda s: land(p.t, s), (s0, s1))
    gate_move = Exchange(p, lambda d: gates.at[d], lambda s: gates_out.at[s], (g0, g1))
    message_move = Exchange(p, lambda d: message.at[d], lambda s: message_out.at[s], (m0, m1))
    spread = Spread(p, land, (ys, yr, ps, pr))
    slot_move.start()
    gate_move.start()
    message_move.start()
    for k in range(n_ep):
        slot_move.wait_arrival(k)
        spread.first(p.ep(k))
    for load in loads:
        load.wait()
    multiply(p.t, True)
    for k in range(n_ep):
        spread.p_arrival(0, p.ep(k)).wait_recv()
    multiply(p.partner, False)
    for k in range(n_ep):
        spread.relay(p.ep(k))
    for off in range(1, p.ny):
        multiply(p.chip(-off), False)
        for k in range(n_ep):
            spread.p_arrival(off, p.ep(k)).wait_recv()
        multiply(p.y_at(-off) * 2 + (1 - p.c), False)
    gate = gate_act[...]
    hidden[...] = (gate * lax.logistic(gate) * up_act[...]).astype(hidden.dtype)
    for k in range(n_ep):
        gate_move.wait_arrival(k)
        message_move.wait_arrival(k)
        spread.wait_sent(p.ep(k))
    slot_move.wait_sent()
    gate_move.wait_sent()
    message_move.wait_sent()


def homeward_kernel(
    n_ep, n_tp, hidden, down_weight, heads, ret, heads_all,
    partial, down_held, pair, mine, out_y, in_y, final,
    w, h0, h1, a0, a1, r0, r1, q0, q1, ys, yr, ps, pr,
):
    p = Place(n_ep, n_tp)
    ny = p.ny
    width = ret.shape[2]

    def cols(t):
        return pl.ds(pl.multiple_of(t * width, width), width)

    def land(t, s):
        return heads_all.at[t, s]

    load = pltpu.make_async_copy(down_weight, down_held, w.at[0])
    load.start()
    p.barrier()
    head_move = Exchange(p, lambda d: heads.at[d], lambda s: land(p.t, s), (h0, h1))
    spread = Spread(p, land, (ys, yr, ps, pr))
    head_move.start()

    def pair_copy(s, off):
        src = partial.at[s, :, cols(p.y_at(off) * 2 + (1 - p.c))]
        return remote(src, pair.at[s, off], r0.at[s, off], r1.at[s, off], p.e, p.partner)

    def y_copy(s, off, to):
        return remote(
            out_y.at[s, off - 1], in_y.at[s, off - 1],
            q0.at[s, off - 1], q1.at[s, off - 1], p.e, p.chip(to),
        )

    def final_copy(k):
        d = p.ep(k)
        return remote(final.at[d], ret.at[p.e], a0.at[d], a1.at[p.e], d, p.t)

    order = list(range(1, n_ep)) + [0]
    capacity = ret.shape[1]

    def multiply(t):
        product = jnp.dot(
            hidden[...], down_held[:, cols(t)], preferred_element_type=jnp.float32
        )
        partial[:, :, cols(t)] = product.astype(jnp.bfloat16).reshape(n_ep, capacity, width)

    load.wait()
    turns = [*range(1, ny), 0]
    for off in turns:
        multiply(p.y_at(off) * 2 + (1 - p.c))
        multiply(p.chip(off))
        for k in order:
            pair_copy(p.ep(k), off).start()
        for k in order:
            s = p.ep(k)
            pair_copy(s, off).wait_recv()
            both = partial[s, :, cols(p.chip(off))].astype(jnp.float32) + pair[s, off].astype(
                jnp.float32
            )
            if off == 0:
                mine[s] = both
            else:
                out_y[s, off - 1] = both.astype(jnp.bfloat16)
                y_copy(s, off, off).start()
    for k in range(n_ep):
        head_move.wait_arrival(k)
        spread.first(p.ep(k))
    for k in order:
        s = p.ep(k)
        total = mine[s]
        for off in range(1, ny):
            y_copy(s, off, -off).wait_recv()
            total = total + in_y[s, off - 1].astype(jnp.float32)
        if k == 0:
            ret[s] = total.astype(jnp.bfloat16)
        else:
            final[s] = total.astype(jnp.bfloat16)
            final_copy(k).start()
    for k in range(n_ep):
        spread.relay(p.ep(k))
    for k in range(n_ep):
        spread.finish(p.ep(k))
    for k in range(n_ep):
        s = p.ep(k)
        for off in range(ny):
            pair_copy(s, off).wait_send()
        for off in range(1, ny):
            y_copy(s, off, off).wait_send()
    for k in range(1, n_ep):
        s = p.ep(k)
        remote(final.at[s], ret.at[s], a0.at[s], a1.at[s], s, p.t).wait_recv()
        final_copy(k).wait_send()
    head_move.wait_sent()


def outward(slots, message, gates, gate_weight, up_weight, n_ep, n_tp):
    _, capacity, width = slots.shape
    rows, units = n_ep * capacity, gate_weight.shape[0]
    scratch = [
        pltpu.VMEM((n_ep, capacity, width * n_tp), slots.dtype),
        pltpu.VMEM(gate_weight.shape, gate_weight.dtype),
        pltpu.VMEM(up_weight.shape, up_weight.dtype),
        pltpu.VMEM((rows, units), jnp.float32),
        pltpu.VMEM((rows, units), jnp.float32),
    ]
    sems = [DMA((n_ep,))] * 6 + [DMA((2,))] + spread_sems(n_ep, n_tp)
    return pl.pallas_call(
        functools.partial(outward_kernel, n_ep, n_tp),
        out_shape=[
            jax.ShapeDtypeStruct((rows, units), slots.dtype),
            jax.ShapeDtypeStruct(message.shape, message.dtype),
            jax.ShapeDtypeStruct(gates.shape, gates.dtype),
        ],
        in_specs=[VM] * 3 + [ANY] * 2,
        out_specs=[VM] * 3,
        scratch_shapes=scratch + sems,
        compiler_params=pltpu.CompilerParams(collective_id=0, has_side_effects=True),
        name="outward",
    )(slots, message, gates, gate_weight, up_weight)


def homeward(hidden, down_weight, heads, n_ep, n_tp):
    capacity, features = hidden.shape[0] // n_ep, down_weight.shape[1]
    width, ny = features // n_tp, n_tp // 2
    far = max(ny - 1, 1)
    scratch = [
        pltpu.VMEM((n_ep, capacity, features), jnp.bfloat16),
        pltpu.VMEM(down_weight.shape, down_weight.dtype),
        pltpu.VMEM((n_ep, ny, capacity, width), jnp.bfloat16),
        pltpu.VMEM((n_ep, capacity, width), jnp.float32),
        pltpu.VMEM((n_ep, far, capacity, width), jnp.bfloat16),
        pltpu.VMEM((n_ep, far, capacity, width), jnp.bfloat16),
        pltpu.VMEM((n_ep, capacity, width), jnp.bfloat16),
    ]
    sems = [DMA((1,))] + [DMA((n_ep,))] * 4 + [DMA((n_ep, ny))] * 2 + [DMA((n_ep, far))] * 2
    return pl.pallas_call(
        functools.partial(homeward_kernel, n_ep, n_tp),
        out_shape=[
            jax.ShapeDtypeStruct((n_ep, capacity, width), jnp.bfloat16),
            jax.ShapeDtypeStruct((n_tp,) + heads.shape, jnp.bfloat16),
        ],
        in_specs=[VM, ANY, VM],
        out_specs=[VM] * 2,
        scratch_shapes=scratch + sems + spread_sems(n_ep, n_tp),
        compiler_params=pltpu.CompilerParams(collective_id=1, has_side_effects=True),
        name="homeward",
    )(hidden, down_weight, heads)


def on_device(
    mixer_tokens,
    mixer_gain,
    query_weight,
    key_weight,
    value_weight,
    forget_weight,
    forget_bias,
    output_weight,
    expert_tokens,
    expert_gain,
    routes,
    route_weights,
    gate_weight,
    up_weight,
    down_weight,
):
    n_ep, n_tp = lax.axis_size("ep"), lax.axis_size("tp")
    rows, features = mixer_tokens.shape
    local_heads = forget_weight.shape[1]
    share = n_ep // local_heads
    part = rows // share
    width = features // n_tp
    bf16, f32 = jnp.bfloat16, jnp.float32

    expert_normed = normed_rows(expert_tokens, expert_gain)
    token_count, top_count = routes.shape
    capacity = 2 * top_count * token_count // n_ep
    pairs = token_count * top_count
    flat_routes = routes.reshape(-1)
    onehot = flat_routes[:, None] == jnp.arange(n_ep, dtype=jnp.int32)[None, :]
    before = jnp.tril(jnp.ones((pairs, pairs), bf16), -1)
    ranks = jnp.dot(before, onehot.astype(bf16), preferred_element_type=f32)
    slot_rank = jnp.sum(jnp.where(onehot, ranks, 0.0), axis=1).astype(jnp.int32)
    slot_index = (flat_routes * capacity + slot_rank).reshape(token_count, top_count)
    slot_ids = jnp.arange(n_ep * capacity, dtype=jnp.int32)
    picks = [(slot_index[:, j][:, None] == slot_ids[None, :]).astype(bf16) for j in range(top_count)]
    column = lax.axis_index("tp") * width
    own_columns = lax.dynamic_slice_in_dim(expert_normed, column, width, 1)
    slots = lax.dot_general(
        sum(picks[1:], picks[0]), own_columns, (((0,), (0,)), ((), ())),
        preferred_element_type=f32,
    ).astype(bf16).reshape(n_ep, capacity, width)

    normed = normed_rows(mixer_tokens, mixer_gain)
    queries = by_rows(normed, query_weight).astype(bf16)
    key_rows = by_rows(normed, key_weight).astype(bf16)
    value_rows = by_rows(normed, value_weight).astype(bf16)
    pre_gate = jnp.dot(normed, forget_weight, preferred_element_type=f32) + forget_bias
    block_cum = jnp.dot(
        jnp.tril(jnp.ones((rows, rows), f32)), jax.nn.log_sigmoid(pre_gate),
        precision=lax.Precision.HIGHEST, preferred_element_type=f32,
    )
    key_value = jnp.concatenate(
        [
            key_rows.reshape(rows, local_heads, HD).transpose(1, 0, 2),
            value_rows.reshape(rows, local_heads, HD).transpose(1, 0, 2),
        ],
        axis=2,
    )
    key_value = jnp.broadcast_to(
        key_value[:, None], (local_heads, share, rows, 2 * HD)
    ).reshape(n_ep, rows, 2 * HD)
    half = part // 2
    query_parts = queries.reshape(share, 2, half, local_heads, HD).transpose(3, 0, 2, 1, 4)
    query_parts = query_parts.reshape(n_ep, half, 2 * HD)
    message = jnp.concatenate([key_value, query_parts], axis=1)
    gates = jnp.broadcast_to(block_cum.T[:, None, None, :], (local_heads, share, 1, rows))
    gates = gates.reshape(n_ep, 1, rows)

    hidden, all_messages, all_gates = outward(
        slots, message, gates, gate_weight[0], up_weight[0], n_ep, n_tp
    )

    positions = n_ep * rows
    all_gates = all_gates.reshape(n_ep, rows)
    totals = all_gates[:, rows - 1]
    lower = jnp.arange(n_ep)[None, :] < jnp.arange(n_ep)[:, None]
    base = jnp.sum(jnp.where(lower, totals[None, :], 0.0), axis=1)
    cumulative = all_gates + base[:, None]
    keys = all_messages[:, :rows, :HD].reshape(positions, HD)
    values = all_messages[:, :rows, HD:].reshape(positions, HD)
    head_query = all_messages[:, rows:].reshape(n_ep, half, 2, HD).transpose(0, 2, 1, 3)
    head_query = head_query.reshape(n_ep * part, HD)
    first = (lax.axis_index("ep") % share) * part
    query_cum = lax.dynamic_slice_in_dim(cumulative, first, part, 1).reshape(-1)
    query_pos = (
        jnp.arange(n_ep, dtype=jnp.int32)[:, None] * rows
        + first
        + jnp.arange(part, dtype=jnp.int32)[None, :]
    ).reshape(-1)
    key_pos = jnp.arange(positions, dtype=jnp.int32)
    scores = by_rows(head_query, keys) * HD ** (-0.5)
    scores = scores + query_cum[:, None] - cumulative.reshape(-1)[None, :]
    scores = jnp.where(key_pos[None, :] <= query_pos[:, None], scores, -jnp.inf)
    weights = jnp.exp(scores - jnp.max(scores, axis=-1, keepdims=True)).astype(bf16)
    attended = jnp.dot(weights, values, preferred_element_type=f32)
    rescale = lax.rsqrt(jnp.mean(attended * attended, axis=-1, keepdims=True) + HEAD_FLOOR)
    head_out = (attended * rescale).astype(bf16).reshape(n_ep, part, HD)

    returned, heads_all = homeward(hidden, down_weight[0], head_out, n_ep, n_tp)

    heads_all = heads_all.reshape(n_tp, local_heads, share, part, HD).transpose(2, 3, 0, 1, 4)
    heads_all = heads_all.reshape(rows, n_tp * local_heads * HD)
    mixer_output = jnp.dot(heads_all, output_weight, preferred_element_type=f32).astype(bf16)
    returned = returned.reshape(n_ep * capacity, width)
    expert_output = 0.0
    for j in range(top_count):
        picked = jnp.dot(picks[j], returned, preferred_element_type=f32)
        expert_output = expert_output + picked * route_weights[:, j][:, None]
    return (mixer_output, expert_output.astype(bf16))


def solution(mesh):
    in_specs = (
        P("ep", None),
        P(),
        P("tp", None),
        P("tp", None),
        P("tp", None),
        P(None, "tp"),
        P("ep", "tp"),
        P(None, "tp"),
        P("ep", None),
        P(),
        P("ep", None),
        P("ep", None),
        P("ep", "tp", None),
        P("ep", "tp", None),
        P("ep", "tp", None),
    )
    out_specs = (P("ep", "tp"), P("ep", "tp"))
    return jax.shard_map(
        on_device, mesh=mesh, in_specs=in_specs, out_specs=out_specs, check_vma=False
    )
```
